32 devices in a mesh: fs: 8 (over z, y), tp: 4 (over x, core).
Axes of the slice: x: 2, y: 2, z: 4, core: 2. Of those that a mesh axis runs over, the one named last changes fastest.
Arguments:
- prompt: bfloat16 [4096, 2048], P(('fs', 'tp')), may hold values from -6 to 6
- norm_gain: float32 [2048], P('fs'), may hold values from 0.1 to 1.9
- up_trained: float32 [2048, 8192], P('fs', 'tp'), may hold values from -0.125 to 0.125
- down_trained: float32 [2048, 8192], P('fs', 'tp'), may hold values from -0.0625 to 0.0625
Outputs:
- up_served: bfloat16 [2048, 8192], P(None, 'tp')
- down_served: bfloat16 [8192, 2048], P('tp')
- mixed: bfloat16 [4096, 2048], P(('fs', 'tp'))
The draws below stay inside these ranges and needn't reach their ends.
All inputs are finite; a program needn't handle non-finite values.
Results may differ from the reference program's by a relative error of at most 0.014.
Values may be sent and summed in bfloat16 or wider, within the bound.
A program may use at most 128 MiB of HBM per device.

```python
import jax
import jax.numpy as jnp
from jax import lax

D = 2048
FF = 8192
TOK_DEV = 128
TOKENS = 4096
N_FS = 8
N_TP = 4


def steps_of(rng, extent, split, least, high):
    def one(position, shards_of):
        steps = jax.random.uniform(jax.random.fold_in(jax.random.fold_in(rng, 6), position), (shards_of,), jnp.float32, least / len(split), high / len(split))
        return jnp.repeat(jnp.exp(steps), extent[position] // shards_of).reshape((-1,) + (1,) * (len(extent) - position - 1))

    loudness = one(*split[0])
    for cut in split[1:]:
        loudness = loudness * one(*cut)
    return loudness


def gaussian(stream_key, shape, deviation, reach, shards=(), kind=jnp.bfloat16):
    entries = jax.random.normal(stream_key, shape, jnp.float32) * deviation
    if len(shards) > 0:
        entries = steps_of(stream_key, shape, shards, -0.22, 0.18) * entries
    return jnp.clip(entries, min=-reach, max=reach).astype(kind)


def setup_inputs(seed: int = 0) -> dict:
    key_of = jax.random.split(jax.random.key(seed), 5)
    return {
        "prompt": gaussian(key_of[0], (TOKENS, D), 1.0, 6.0, ((0, 32),)),
        "norm_gain": jnp.clip(1.0 + 0.18 * jax.random.normal(key_of[1], (D,), jnp.float32), 0.1, 1.9),
        "up_trained": gaussian(key_of[2], (D, FF), D ** -0.5, 0.125, ((0, 8), (1, 4)), jnp.float32),
        "down_trained": gaussian(key_of[3], (D, FF), FF ** -0.5, 0.0625, ((0, 8), (1, 4)), jnp.float32),
    }


def reference(prompt, norm_gain, up_trained, down_trained):
    up_served = (norm_gain[:, None] * up_trained).astype(jnp.bfloat16)
    down_served = jnp.transpose(down_trained).astype(jnp.bfloat16)
    width = FF // N_TP
    groups = prompt.reshape(N_FS, N_TP * TOK_DEV, D)

    def one_group(rows):
        values = rows.astype(jnp.float32)
        scale = lax.rsqrt(lax.optimization_barrier(jnp.mean(values * values, axis=-1, keepdims=True)) + 1e-06)
        normed = (values * scale).astype(jnp.bfloat16)
        pre = jnp.dot(normed, up_served, preferred_element_type=jnp.float32)
        hidden = jnp.square(jax.nn.relu(pre)).astype(jnp.bfloat16)
        total = jnp.zeros((rows.shape[0], D), jnp.float32)
        for block in range(N_TP):
            partial_value = jnp.dot(hidden[:, block * width:(block + 1) * width], down_served[block * width:(block + 1) * width, :], preferred_element_type=jnp.float32).astype(jnp.bfloat16)
            total = total + partial_value.astype(jnp.float32)
        return total.astype(jnp.bfloat16)
    mixed = lax.map(one_group, groups).reshape(TOKENS, D)
    return (up_served, down_served, mixed)
```

```python
import functools

import jax
import jax.numpy as jnp
from jax import lax
from jax.experimental import pallas as pl
from jax.experimental.pallas import tpu as pltpu
from jax.sharding import PartitionSpec as P

MESH = pl.DeviceIdType.MESH
PIECES = 2
LIMIT = 40
LANES = 128


def factor(fs):
    ny = 1
    while ny * 2 * ny * 2 <= fs:
        ny *= 2
    return fs // ny, ny


def turns(rows):
    return rows % 128 == 0


def flush(up_in, down_in, mixed_in, up_out, down_out, mixed_out, sems):
    copies = [
        pltpu.make_async_copy(source, target, sems.at[i])
        for i, (source, target) in enumerate(((up_in, up_out), (down_in, down_out), (mixed_in, mixed_out)))
    ]
    for copy in copies:
        copy.start()
    for copy in copies:
        copy.wait()


def kernel(nz, ny, tp, prompt_hbm, gain_hbm, up_hbm, down_hbm, up_all, down_out, mixed,
           prompt, gain_row, gain, up_f, down_f,
           down_scratch, norm_all, hidden, part_send, part_recv,
           in_sems, w_send, w_recv, n_send, n_recv, p_send, p_recv):
    fs = nz * ny
    rows, width = up_f.shape
    tile = 256
    turned = turns(rows)
    down_all = down_scratch if turned else down_out
    piece = rows // PIECES
    tokens = prompt.shape[0]
    me = lax.axis_index("fs")
    t = lax.axis_index("tp")
    z, y = me // ny, lax.rem(me, ny)
    exists = (z < nz - 1, z > 0, y < ny - 1, y > 0)
    step = (ny, -ny, 1, -1)
    trick = ny == 2 and nz % 2 == 0
    half = PIECES // 2
    even = lax.rem(z, 2) == 0
    mate = z + 1 - 2 * lax.rem(z, 2)
    buffers = (up_all, down_all)
    sent = []

    reads = [pltpu.make_async_copy(gain_hbm, gain_row, in_sems.at[0])]
    for c in range(PIECES):
        part = pl.ds(c * piece, piece)
        reads.append(pltpu.make_async_copy(up_hbm.at[part], up_f.at[part], in_sems.at[1 + c]))
    reads.append(pltpu.make_async_copy(prompt_hbm, prompt, in_sems.at[1 + PIECES]))
    reads.append(pltpu.make_async_copy(down_hbm, down_f, in_sems.at[2 + PIECES]))
    for read in reads:
        read.start()

    barrier = pltpu.get_barrier_semaphore()
    for direction in range(4):
        @pl.when(exists[direction])
        def _():
            pl.semaphore_signal(barrier, inc=1, device_id={"fs": me + step[direction]}, device_id_type=MESH)
    for offset in range(1, tp):
        pl.semaphore_signal(barrier, inc=1, device_id={"tp": lax.rem(t + offset, tp)}, device_id_type=MESH)

    def weights(phase, block, c, direction):
        start = pl.multiple_of(block * rows + c * piece, piece)
        ref = buffers[phase].at[pl.ds(start, piece)]
        slot = (phase * fs + block) * PIECES + c
        return pltpu.make_async_remote_copy(
            src_ref=ref, dst_ref=ref,
            send_sem=w_send.at[direction, slot], recv_sem=w_recv.at[slot],
            device_id={"fs": me + step[direction]}, device_id_type=MESH)

    def send(condition, phase, block, c, direction):
        condition = jnp.logical_and(condition, exists[direction])
        sent.append((condition, phase, block, c, direction))

        @pl.when(condition)
        def _():
            weights(phase, block, c, direction).start()

    def arrive(condition, phase, block, c):
        @pl.when(condition)
        def _():
            weights(phase, block, c, 0).wait_recv()

    reads[0].wait()
    gain[...] = jnp.transpose(jnp.broadcast_to(gain_row[...], (LANES, rows)))
    always = z >= 0
    for c in range(PIECES):
        reads[1 + c].wait()
        where = pl.ds(pl.multiple_of(me * rows + c * piece, piece), piece)
        part = slice(c * piece, (c + 1) * piece)
        for k in range(0, width, LANES):
            up_all[where, k:k + LANES] = (gain[part, :] * up_f[part, k:k + LANES]).astype(jnp.bfloat16)
        if c == 0:
            pl.semaphore_wait(barrier, sum(e.astype(jnp.int32) for e in exists) + tp - 1)
        for direction in range(4):
            send(always, 0, me, c, direction)

    reads[1 + PIECES].wait()
    values = prompt[...].astype(jnp.float32)
    scale = lax.rsqrt(jnp.mean(values * values, axis=-1, keepdims=True) + 1e-06)
    mine = pl.ds(pl.multiple_of(t * tokens, tokens), tokens)
    norm_all[mine, :] = (values * scale).astype(jnp.bfloat16)
    reads[2 + PIECES].wait()
    for c in range(PIECES):
        where = pl.ds(pl.multiple_of(me * rows + c * piece, piece), piece)
        part = slice(c * piece, (c + 1) * piece)
        down_all[where, :] = down_f[part, :].astype(jnp.bfloat16)

    def token_copy(offset):
        return pltpu.make_async_remote_copy(
            src_ref=norm_all.at[mine], dst_ref=norm_all.at[mine],
            send_sem=n_send.at[offset], recv_sem=n_recv.at[t],
            device_id={"tp": lax.rem(t + offset, tp)}, device_id_type=MESH)

    def token_arrival(offset):
        source = lax.rem(t + offset, tp)
        ref = norm_all.at[pl.ds(pl.multiple_of(source * tokens, tokens), tokens)]
        return pltpu.make_async_remote_copy(
            src_ref=ref, dst_ref=ref, send_sem=n_send.at[offset], recv_sem=n_recv.at[source],
            device_id={"tp": source}, device_id_type=MESH)

    for offset in range(1, tp):
        token_copy(offset).start()
    for c in range(half):
        for direction in (2, 3):
            send(always, 1, me, c, direction)

    def own_down(d):
        for c in range(PIECES):
            send(z == d, 1, me, c, 0)
            send(z == nz - 1 - d, 1, me, c, 1)

    def column(phase, d):
        for c in range(PIECES):
            for s in (1, -1):
                zb = z + s * d
                there = jnp.logical_and(zb >= 0, zb < nz)
                block = zb * ny + y
                arrive(there, phase, block, c)
                send(there, phase, block, c, 1 if s > 0 else 0)
                across = there
                if trick and c >= half:
                    across = jnp.logical_and(there, zb != mate)
                send(across, phase, block, c, 2)
                send(across, phase, block, c, 3)

    def swap(phase):
        if not trick:
            return
        block = z * ny + 1 - y
        for c in range(half, PIECES):
            if phase == 0:
                arrive(always, phase, block, c)
            send(even, phase, block, c, 0)
            send(jnp.logical_not(even), phase, block, c, 1)

    def sideways(phase, d, s):
        zb = z + s * d
        inside = jnp.logical_and(zb >= 0, zb < nz)
        for e in range(1, ny):
            for u in (1, -1):
                yb = y + u * e
                there = jnp.logical_and(inside, jnp.logical_and(yb >= 0, yb < ny))
                for c in range(PIECES):
                    if trick and phase == 0 and d == 0 and c >= half:
                        continue
                    wanted = there
                    if trick and c >= half:
                        wanted = jnp.logical_and(there, zb != mate)
                    arrive(wanted, phase, zb * ny + yb, c)
                    if e < ny - 1:
                        send(wanted, phase, zb * ny + yb, c, 3 if u > 0 else 2)

    def swapped(phase):
        if trick:
            for c in range(half, PIECES):
                arrive(always, phase, mate * ny + 1 - y, c)

    def partial_copy(block, offset):
        peer = lax.rem(t + offset, tp)
        return pltpu.make_async_remote_copy(
            src_ref=part_send.at[block, pl.ds(pl.multiple_of(peer * tokens, tokens), tokens)],
            dst_ref=part_recv.at[t, block],
            send_sem=p_send.at[offset], recv_sem=p_recv.at[t],
            device_id={"tp": peer}, device_id_type=MESH)

    def consume(condition, block):
        @pl.when(condition)
        def _():
            where = pl.ds(pl.multiple_of(block * rows, rows), rows)
            part_send[block] = lax.dot_general(
                hidden[...], down_all[where, :], (((1,), (1,)), ((), ())),
                preferred_element_type=jnp.float32).astype(jnp.bfloat16)
            for offset in range(1, tp):
                partial_copy(block, offset).start()
            if turned:
                @pl.loop(0, width // tile)
                def _(j):
                    at = pl.ds(pl.multiple_of(j * tile, tile), tile)
                    down_out[at, where] = jnp.transpose(down_all[where, at])

    def consume_column(d):
        @pl.loop(0, 1 if d == 0 else 2)
        def _(i):
            zb = z + (1 - 2 * i) * d
            consume(jnp.logical_and(zb >= 0, zb < nz), zb * ny + y)

    def consume_sideways(d):
        @pl.loop(0, (1 if d == 0 else 2) * (ny - 1))
        def _(i):
            zb = z + (1 - 2 * (i // (ny - 1))) * d
            yb = lax.rem(y + 1 + lax.rem(i, ny - 1), ny)
            inside = jnp.logical_and(zb >= 0, zb < nz)
            if trick:
                inside = jnp.logical_and(inside, zb != mate)
            consume(inside, zb * ny + yb)

    def signs(d):
        return (1,) if d == 0 else (1, -1)

    own_down(0)
    for d in range(1, nz):
        column(0, d)
        if d == 1:
            swap(0)
        own_down(d)
    for c in range(half, PIECES):
        for direction in (2, 3):
            send(always, 1, me, c, direction)
    for d in range(nz):
        for s in signs(d):
            sideways(0, d, s)
    swapped(0)
    for offset in range(1, tp):
        token_arrival(offset).wait_recv()

    @pl.loop(0, width // tile)
    def _(j):
        at = pl.ds(pl.multiple_of(j * tile, tile), tile)
        pre = jnp.dot(norm_all[...], up_all[:, at], preferred_element_type=jnp.float32)
        hidden[:, at] = jnp.square(jnp.maximum(pre, 0.0)).astype(jnp.bfloat16)

    for d in range(1, nz):
        column(1, d)
        if d == nz - 1:
            swap(1)
        consume_column(d - 1)
        if d == 1:
            sideways(1, 0, 1)
            consume_sideways(0)
    if nz == 1:
        sideways(1, 0, 1)
        consume_sideways(0)
    consume_column(nz - 1)
    for d in range(1, nz):
        for s in signs(d):
            sideways(1, d, s)
        consume_sideways(d)
    if trick:
        swapped(1)
        consume(always, mate * ny + 1 - y)

    for offset in range(1, tp):
        source = lax.rem(t + offset, tp)
        whole = part_recv.at[source]
        arrival = pltpu.make_async_remote_copy(
            src_ref=whole, dst_ref=whole, send_sem=p_send.at[offset], recv_sem=p_recv.at[source],
            device_id={"tp": source}, device_id_type=MESH)
        arrival.wait_recv()
    for block in range(fs):
        total = part_send[block, mine, :].astype(jnp.float32)
        for offset in range(1, tp):
            total += part_recv[lax.rem(t + offset, tp), block].astype(jnp.float32)
        mixed[:, block * rows:(block + 1) * rows] = total.astype(jnp.bfloat16)

    for offset in range(1, tp):
        token_copy(offset).wait_send()
        whole = part_recv.at[t]
        pltpu.make_async_remote_copy(
            src_ref=whole, dst_ref=whole, send_sem=p_send.at[offset], recv_sem=p_recv.at[t],
            device_id={"tp": lax.rem(t + offset, tp)}, device_id_type=MESH).wait_send()
    for condition, phase, block, c, direction in sent:
        @pl.when(condition)
        def _():
            weights(phase, block, c, direction).wait_send()


def solution(mesh):
    fs, tp = mesh.shape["fs"], mesh.shape["tp"]
    nz, ny = factor(fs)

    def shards(prompt, norm_gain, up_trained, down_trained):
        rows, width = up_trained.shape
        tokens, depth = prompt.shape
        bf16 = jnp.bfloat16
        turned = turns(rows)
        down_shape = (width, depth) if turned else (depth, width)
        slots = 2 * fs * PIECES
        any_space = pl.BlockSpec(memory_space=pl.ANY)
        vmem = pl.BlockSpec(memory_space=pltpu.VMEM)
        up_whole, down_whole, mixed = pl.pallas_call(
            functools.partial(kernel, nz, ny, tp),
            out_shape=(
                pltpu.VMEM((depth, width), bf16),
                pltpu.VMEM(down_shape, bf16),
                pltpu.VMEM((tokens, depth), bf16),
            ),
            in_specs=[any_space] * 4,
            out_specs=[vmem] * 3,
            scratch_shapes=[
                pltpu.VMEM((tokens, depth), bf16),
                pltpu.VMEM((1, rows), jnp.float32),
                pltpu.VMEM((rows, LANES), jnp.float32),
                pltpu.VMEM((rows, width), jnp.float32),
                pltpu.VMEM((rows, width), jnp.float32),
                pltpu.VMEM((depth, width) if turned else (16, 128), bf16),
                pltpu.VMEM((tp * tokens, depth), bf16),
                pltpu.VMEM((tp * tokens, width), bf16),
                pltpu.VMEM((fs, tp * tokens, rows), bf16),
                pltpu.VMEM((tp, fs, tokens, rows), bf16),
                pltpu.SemaphoreType.DMA((3 + PIECES,)),
                pltpu.SemaphoreType.DMA((4, slots)),
                pltpu.SemaphoreType.DMA((slots,)),
                pltpu.SemaphoreType.DMA((tp,)),
                pltpu.SemaphoreType.DMA((tp,)),
                pltpu.SemaphoreType.DMA((tp,)),
                pltpu.SemaphoreType.DMA((tp,)),
            ],
            compiler_params=pltpu.CompilerParams(
                collective_id=0, has_side_effects=True, vmem_limit_bytes=LIMIT * 1024 * 1024
            ),
        )(prompt, norm_gain[None, :], up_trained, down_trained)
        up_whole, down_whole, mixed = pl.pallas_call(
            flush,
            out_shape=(
                jax.ShapeDtypeStruct((depth, width), bf16),
                jax.ShapeDtypeStruct(down_shape, bf16),
                jax.ShapeDtypeStruct((tokens, depth), bf16),
            ),
            in_specs=[vmem] * 3,
            out_specs=[any_space] * 3,
            scratch_shapes=[pltpu.SemaphoreType.DMA((3,))],
            compiler_params=pltpu.CompilerParams(vmem_limit_bytes=2 * 1024 * 1024),
        )(up_whole, down_whole, mixed)
        return up_whole, down_whole if turned else jnp.transpose(down_whole), mixed

    return jax.shard_map(
        shards,
        mesh=mesh,
        in_specs=(P(("fs", "tp"), None), P("fs"), P("fs", "tp"), P("fs", "tp")),
        out_specs=(P(None, "tp"), P("tp", None), P(("fs", "tp"), None)),
        check_vma=False,
    )
```

```python
import functools

import jax
import jax.numpy as jnp
from jax import lax
from jax.experimental import pallas as pl
from jax.experimental.pallas import tpu as pltpu
from jax.sharding import PartitionSpec as P

MESH = pl.DeviceIdType.MESH
PIECES = 2
LIMIT = 40
LANES = 128


def factor(fs):
    ny = 1
    while ny * 2 * ny * 2 <= fs:
        ny *= 2
    return fs // ny, ny


def turns(rows):
    return rows % 128 == 0


def units_of(rows):
    return PIECES if rows // PIECES % LANES == 0 else 1


def flush(up_in, down_in, mixed_in, up_out, down_out, mixed_out, sems):
    copies = [
        pltpu.make_async_copy(source, target, sems.at[i])
        for i, (source, target) in enumerate(((up_in, up_out), (down_in, down_out), (mixed_in, mixed_out)))
    ]
    for copy in copies:
        copy.start()
    for copy in copies:
        copy.wait()


def kernel(nz, ny, tp, prompt_hbm, gain_hbm, up_hbm, down_hbm, up_all, down_out, mixed,
           prompt, gain_row, gain, up_f, down_f,
           down_scratch, norm_all, hidden, part_send, part_recv,
           in_sems, w_send, w_recv, n_send, n_recv, p_send, p_recv):
    fs = nz * ny
    rows, width = up_f.shape
    tile = 256
    turned = turns(rows)
    down_all = down_scratch if turned else down_out
    piece = rows // PIECES
    tokens = prompt.shape[0]
    me = lax.axis_index("fs")
    t = lax.axis_index("tp")
    z, y = me // ny, lax.rem(me, ny)
    exists = (z < nz - 1, z > 0, y < ny - 1, y > 0)
    step = (ny, -ny, 1, -1)
    units = units_of(rows)
    span = rows // units
    trick = ny == 2 and nz > 2 and units == PIECES
    half = PIECES // 2
    buffers = (up_all, down_all)

    reads = [pltpu.make_async_copy(gain_hbm, gain_row, in_sems.at[0])]
    for c in range(PIECES):
        part = pl.ds(c * piece, piece)
        reads.append(pltpu.make_async_copy(up_hbm.at[part], up_f.at[part], in_sems.at[1 + c]))
    reads.append(pltpu.make_async_copy(prompt_hbm, prompt, in_sems.at[1 + PIECES]))
    reads.append(pltpu.make_async_copy(down_hbm, down_f, in_sems.at[2 + PIECES]))
    for read in reads:
        read.start()

    barrier = pltpu.get_barrier_semaphore()
    for direction in range(4):
        @pl.when(exists[direction])
        def _():
            pl.semaphore_signal(barrier, inc=1, device_id={"fs": me + step[direction]}, device_id_type=MESH)
    for offset in range(1, tp):
        pl.semaphore_signal(barrier, inc=1, device_id={"tp": lax.rem(t + offset, tp)}, device_id_type=MESH)

    def weights(phase, block, c, direction):
        start = pl.multiple_of(block * rows + c * piece, piece)
        ref = buffers[phase].at[pl.ds(start, piece)]
        slot = (phase * fs + block) * PIECES + c
        return pltpu.make_async_remote_copy(
            src_ref=ref, dst_ref=ref,
            send_sem=w_send.at[direction, phase], recv_sem=w_recv.at[slot],
            device_id={"fs": me + step[direction]}, device_id_type=MESH)

    def send(condition, phase, block, c, direction):
        @pl.when(jnp.logical_and(condition, exists[direction]))
        def _():
            weights(phase, block, c, direction).start()

    def arrive(condition, phase, block, c):
        @pl.when(condition)
        def _():
            weights(phase, block, c, 0).wait_recv()

    reads[0].wait()
    gain[...] = jnp.transpose(jnp.broadcast_to(gain_row[...], (LANES, rows)))
    always = z >= 0
    for c in range(PIECES):
        reads[1 + c].wait()
        where = pl.ds(pl.multiple_of(me * rows + c * piece, piece), piece)
        part = slice(c * piece, (c + 1) * piece)
        for k in range(0, width, LANES):
            up_all[where, k:k + LANES] = (gain[part, :] * up_f[part, k:k + LANES]).astype(jnp.bfloat16)
        if c == 0:
            pl.semaphore_wait(barrier, sum(e.astype(jnp.int32) for e in exists) + tp - 1)
        for direction in range(4):
            send(always, 0, me, c, direction)

    reads[1 + PIECES].wait()
    values = prompt[...].astype(jnp.float32)
    scale = lax.rsqrt(jnp.mean(values * values, axis=-1, keepdims=True) + 1e-06)
    mine = pl.ds(pl.multiple_of(t * tokens, tokens), tokens)
    norm_all[mine, :] = (values * scale).astype(jnp.bfloat16)
    reads[2 + PIECES].wait()
    for c in range(PIECES):
        where = pl.ds(pl.multiple_of(me * rows + c * piece, piece), piece)
        part = slice(c * piece, (c + 1) * piece)
        down_all[where, :] = down_f[part, :].astype(jnp.bfloat16)

    def token_copy(offset):
        return pltpu.make_async_remote_copy(
            src_ref=norm_all.at[mine], dst_ref=norm_all.at[mine],
            send_sem=n_send.at[offset], recv_sem=n_recv.at[t],
            device_id={"tp": lax.rem(t + offset, tp)}, device_id_type=MESH)

    def token_arrival(offset):
        source = lax.rem(t + offset, tp)
        ref = norm_all.at[pl.ds(pl.multiple_of(source * tokens, tokens), tokens)]
        return pltpu.make_async_remote_copy(
            src_ref=ref, dst_ref=ref, send_sem=n_send.at[offset], recv_sem=n_recv.at[source],
            device_id={"tp": source}, device_id_type=MESH)

    for offset in range(1, tp):
        token_copy(offset).start()
    for c in range(half):
        for direction in (2, 3):
            send(always, 1, me, c, direction)

    def own_down(d):
        for c in range(PIECES):
            if trick and c >= half and d == nz - 2:
                continue
            send(z == d, 1, me, c, 0)
            send(z == nz - 1 - d, 1, me, c, 1)

    def own_late():
        if trick:
            for c in range(half, PIECES):
                send(z == nz - 2, 1, me, c, 0)
                send(z == 1, 1, me, c, 1)

    def own_aside():
        for c in range(half, PIECES):
            for direction in (2, 3):
                send(always, 1, me, c, direction)

    def column(phase, d):
        for c in range(PIECES):
            near = trick and c >= half and d == 1
            for s in (1, -1):
                zb = z + s * d
                there = jnp.logical_and(zb >= 0, zb < nz)
                if near and phase == 1:
                    there = jnp.logical_and(there, exists[1 if s > 0 else 0])
                block = zb * ny + y
                arrive(there, phase, block, c)
                send(there, phase, block, c, 1 if s > 0 else 0)
                if not near:
                    send(there, phase, block, c, 2)
                    send(there, phase, block, c, 3)

    def landed():
        for c in range(half, PIECES):
            arrive(z == 0, 1, (z + 1) * ny + y, c)
            arrive(z == nz - 1, 1, (z - 1) * ny + y, c)

    def swap(phase):
        if not trick:
            return
        block = z * ny + 1 - y
        for c in range(half, PIECES):
            if phase == 0:
                arrive(always, phase, block, c)
            send(always, phase, block, c, 0)
            send(always, phase, block, c, 1)

    def sideways(phase, d, s, pieces):
        zb = z + s * d
        inside = jnp.logical_and(zb >= 0, zb < nz)
        for e in range(1, ny):
            for u in (1, -1):
                yb = y + u * e
                there = jnp.logical_and(inside, jnp.logical_and(yb >= 0, yb < ny))
                for c in pieces:
                    if trick and c >= half and (d == 1 or (phase == 0 and d == 0)):
                        continue
                    arrive(there, phase, zb * ny + yb, c)
                    if e < ny - 1:
                        send(there, phase, zb * ny + yb, c, 3 if u > 0 else 2)

    def swapped(phase):
        if trick:
            for c in range(half, PIECES):
                for s in (1, -1):
                    zb = z + s
                    arrive(jnp.logical_and(zb >= 0, zb < nz), phase, zb * ny + 1 - y, c)

    def partial_copy(unit, offset, group):
        peer = lax.rem(t + offset, tp)
        return pltpu.make_async_remote_copy(
            src_ref=part_send.at[unit, pl.ds(pl.multiple_of(peer * tokens, tokens), tokens)],
            dst_ref=part_recv.at[t, unit],
            send_sem=p_send.at[offset], recv_sem=p_recv.at[t, group],
            device_id={"tp": peer}, device_id_type=MESH)

    def arrivals(group, count):
        for offset in range(1, tp):
            source = lax.rem(t + offset, tp)
            ref = part_recv.at[source, pl.ds(0, count)]
            pltpu.make_async_remote_copy(
                src_ref=ref, dst_ref=ref, send_sem=p_send.at[offset], recv_sem=p_recv.at[source, group],
                device_id={"tp": source}, device_id_type=MESH).wait_recv()

    def multiply(condition, block, u, group=0):
        @pl.when(condition)
        def _():
            where = pl.ds(pl.multiple_of(block * rows + u * span, span), span)
            unit = block * units + u
            part_send[unit] = lax.dot_general(
                hidden[...], down_all[where, :], (((1,), (1,)), ((), ())),
                preferred_element_type=jnp.float32).astype(jnp.bfloat16)
            for offset in range(1, tp):
                partial_copy(unit, offset, group).start()

    def turn(condition, block, u):
        if not turned:
            return

        @pl.when(condition)
        def _():
            where = pl.ds(pl.multiple_of(block * rows + u * span, span), span)

            @pl.loop(0, width // tile)
            def _(j):
                at = pl.ds(pl.multiple_of(j * tile, tile), tile)
                down_out[at, where] = jnp.transpose(down_all[where, at])

    def consume(condition, block, u):
        multiply(condition, block, u)
        turn(condition, block, u)

    def total_of(unit):
        total = part_send[unit, mine, :].astype(jnp.float32)
        for offset in range(1, tp):
            total += part_recv[lax.rem(t + offset, tp), unit].astype(jnp.float32)
        return total.astype(jnp.bfloat16)

    def add(condition, block, u):
        @pl.when(condition)
        def _():
            unit = block * units + u
            mixed[:, pl.ds(pl.multiple_of(unit * span, span), span)] = total_of(unit)

    def walk(action, d, aside, first, count):
        across = ny - 1 if aside else 1
        if across * count == 0:
            return

        @pl.loop(0, (1 if d == 0 else 2) * across * count)
        def _(i):
            k = i // count
            zb = z + (1 - 2 * (k // across)) * d
            yb = lax.rem(y + 1 + lax.rem(k, across), ny) if aside else y
            action(jnp.logical_and(zb >= 0, zb < nz), zb * ny + yb, first + lax.rem(i, count))

    pending = []

    def use(*place):
        walk(consume, *place)
        pending.append(place)

    def finish():
        if span % LANES == 0:
            for place in pending:
                walk(add, *place)
        pending.clear()

    def use_aside(d, first, count):
        for s in signs(d):
            sideways(1, d, s, range(PIECES) if units == 1 else range(first, first + count))
        use(d, True, first, count)

    def signs(d):
        return (1,) if d == 0 else (1, -1)

    def ready(d):
        use(d, False, 0, half if trick and d == 1 else units)
        if d > 0:
            use_aside(d - 1, 0, half if trick and d == 2 else units)

    own_down(0)
    for d in range(1, nz):
        column(0, d)
        if d == 1:
            swap(0)
        own_down(d)
        if d == nz // 2:
            own_aside()
    if nz == 1:
        own_aside()
    else:
        column(1, 1)
    for d in range(nz):
        for s in signs(d):
            sideways(0, d, s, range(PIECES))
    swapped(0)
    for offset in range(1, tp):
        token_arrival(offset).wait_recv()

    @pl.loop(0, width // tile)
    def _(j):
        at = pl.ds(pl.multiple_of(j * tile, tile), tile)
        pre = jnp.dot(norm_all[...], up_all[:, at], preferred_element_type=jnp.float32)
        hidden[:, at] = jnp.square(jnp.maximum(pre, 0.0)).astype(jnp.bfloat16)

    for d in range(min(nz, 2), nz):
        column(1, d)
        if d == nz - 1:
            own_late()
            swap(1)
        if d == 2:
            ready(0)
            ready(1)
        ready(d)
    if nz <= 2:
        for d in range(nz):
            ready(d)
    if trick:
        landed()
        use(1, False, half, units - half)
    if units > 1:
        use_aside(nz - 1, 0, units - 1)
    late = 2 * (units - half) if trick else 0
    ends = multiply
    if trick:
        arrivals(0, fs * units - late)
        finish()
        ends = functools.partial(multiply, group=1)
    last = [(nz - 1, True, units - 1, 1)]
    for s in signs(nz - 1):
        sideways(1, nz - 1, s, range(PIECES) if units == 1 else range(units - 1, units))
    walk(ends, *last[0])
    if trick:
        swapped(1)
        last.append((1, True, half, units - half))
        walk(ends, *last[1])
    for place in last:
        walk(turn, *place)
        pending.append(place)
    arrivals(1 if trick else 0, late if trick else fs * units)
    finish()
    if span % LANES:
        for block in range(fs):
            mixed[:, block * rows:(block + 1) * rows] = total_of(block)

    for offset in range(1, tp):
        token_copy(offset).wait_send()

    for offset in range(1, tp):
        whole = part_recv.at[t]
        pltpu.make_async_remote_copy(
            src_ref=whole, dst_ref=whole, send_sem=p_send.at[offset], recv_sem=p_recv.at[t, 0],
            device_id={"tp": lax.rem(t + offset, tp)}, device_id_type=MESH).wait_send()

    def drain(condition, direction, pieces):
        @pl.when(jnp.logical_and(condition, exists[direction]))
        def _():
            for phase in range(2):
                ref = buffers[phase].at[pl.ds(0, pieces * piece)]
                pltpu.make_async_remote_copy(
                    src_ref=ref, dst_ref=ref, send_sem=w_send.at[direction, phase], recv_sem=w_recv.at[0],
                    device_id={"fs": me + step[direction]}, device_id_type=MESH).wait_send()

    spare = PIECES - half if trick else 0
    for k in range(nz):
        drain(z == k, 0, (k + 1) * PIECES + spare)
        drain(z == k, 1, (nz - k) * PIECES + spare)
        less = spare * ((k > 0) + (k < nz - 1))
        for e in range(ny):
            here = jnp.logical_and(z == k, y == e)
            drain(here, 2, (e + 1) * nz * PIECES - less)
            drain(here, 3, (ny - e) * nz * PIECES - less)


def solution(mesh):
    fs, tp = mesh.shape["fs"], mesh.shape["tp"]
    nz, ny = factor(fs)

    def shards(prompt, norm_gain, up_trained, down_trained):
        rows, width = up_trained.shape
        tokens, depth = prompt.shape
        bf16 = jnp.bfloat16
        turned = turns(rows)
        down_shape = (width, depth) if turned else (depth, width)
        slots = 2 * fs * PIECES
        parts = fs * units_of(rows)
        any_space = pl.BlockSpec(memory_space=pl.ANY)
        vmem = pl.BlockSpec(memory_space=pltpu.VMEM)
        up_whole, down_whole, mixed = pl.pallas_call(
            functools.partial(kernel, nz, ny, tp),
            out_shape=(
                pltpu.VMEM((depth, width), bf16),
                pltpu.VMEM(down_shape, bf16),
                pltpu.VMEM((tokens, depth), bf16),
            ),
            in_specs=[any_space] * 4,
            out_specs=[vmem] * 3,
            scratch_shapes=[
                pltpu.VMEM((tokens, depth), bf16),
                pltpu.VMEM((1, rows), jnp.float32),
                pltpu.VMEM((rows, LANES), jnp.float32),
                pltpu.VMEM((rows, width), jnp.float32),
                pltpu.VMEM((rows, width), jnp.float32),
                pltpu.VMEM((depth, width) if turned else (16, 128), bf16),
                pltpu.VMEM((tp * tokens, depth), bf16),
                pltpu.VMEM((tp * tokens, width), bf16),
                pltpu.VMEM((parts, tp * tokens, depth // parts), bf16),
                pltpu.VMEM((tp, parts, tokens, depth // parts), bf16),
                pltpu.SemaphoreType.DMA((3 + PIECES,)),
                pltpu.SemaphoreType.DMA((4, 2)),
                pltpu.SemaphoreType.DMA((slots,)),
                pltpu.SemaphoreType.DMA((tp,)),
                pltpu.SemaphoreType.DMA((tp,)),
                pltpu.SemaphoreType.DMA((tp,)),
                pltpu.SemaphoreType.DMA((tp, 2)),
            ],
            compiler_params=pltpu.CompilerParams(
                collective_id=0, has_side_effects=True, vmem_limit_bytes=LIMIT * 1024 * 1024
            ),
        )(prompt, norm_gain[None, :], up_trained, down_trained)
        up_whole, down_whole, mixed = pl.pallas_call(
            flush,
            out_shape=(
                jax.ShapeDtypeStruct((depth, width), bf16),
                jax.ShapeDtypeStruct(down_shape, bf16),
                jax.ShapeDtypeStruct((tokens, depth), bf16),
            ),
            in_specs=[vmem] * 3,
            out_specs=[any_space] * 3,
            scratch_shapes=[pltpu.SemaphoreType.DMA((3,))],
            compiler_params=pltpu.CompilerParams(vmem_limit_bytes=2 * 1024 * 1024),
        )(up_whole, down_whole, mixed)
        return up_whole, down_whole if turned else jnp.transpose(down_whole), mixed

    return jax.shard_map(
        shards,
        mesh=mesh,
        in_specs=(P(("fs", "tp"), None), P("fs"), P("fs", "tp"), P("fs", "tp")),
        out_specs=(P(None, "tp"), P("tp", None), P(("fs", "tp"), None)),
        check_vma=False,
    )
```

```python
import functools

import jax
import jax.numpy as jnp
from jax import lax
from jax.experimental import pallas as pl
from jax.experimental.pallas import tpu as pltpu
from jax.sharding import PartitionSpec as P

MESH = pl.DeviceIdType.MESH
PIECES = 2
LIMIT = 40
LANES = 128
CUTS = 4
TURN = 128 * 1024


def factor(fs):
    ny = 1
    while ny * 2 * ny * 2 <= fs:
        ny *= 2
    return fs // ny, ny


def turns(rows):
    return rows % 128 == 0


def units_of(rows):
    return PIECES if rows // PIECES % LANES == 0 else 1


def flush(up_in, down_in, mixed_in, up_out, down_out, mixed_out, sems):
    copies = [
        pltpu.make_async_copy(source, target, sems.at[i])
        for i, (source, target) in enumerate(((up_in, up_out), (down_in, down_out), (mixed_in, mixed_out)))
    ]
    for copy in copies:
        copy.start()
    for copy in copies:
        copy.wait()


def kernel(nz, ny, tp, prompt_hbm, gain_hbm, up_hbm, down_hbm, up_all, down_out, mixed,
           prompt, gain_row, gain, up_f, down_f,
           down_scratch, norm_all, hidden, part_send, part_recv, late_send, late_recv,
           in_sems, w_send, w_recv, w_late, n_send, n_recv, p_send, p_recv):
    fs = nz * ny
    rows, width = up_f.shape
    tile = 256
    turned = turns(rows)
    down_all = down_scratch if turned else down_out
    piece = rows // PIECES
    tokens = prompt.shape[0]
    me = lax.axis_index("fs")
    t = lax.axis_index("tp")
    z, y = me // ny, lax.rem(me, ny)
    exists = (z < nz - 1, z > 0, y < ny - 1, y > 0)
    step = (ny, -ny, 1, -1)
    units = units_of(rows)
    span = rows // units
    trick = ny == 2 and nz > 2 and units == PIECES == 2 and tokens % LANES == 0
    cut = piece // CUTS
    opening = CUTS if cut % 16 == 0 else 1
    half = PIECES // 2
    buffers = (up_all, down_all)

    bounds = [(k * piece // opening, piece // opening) for k in range(opening)]
    bounds += [(c * piece, piece) for c in range(1, PIECES)]
    reads = [pltpu.make_async_copy(gain_hbm, gain_row, in_sems.at[0])]
    for k, (start, size) in enumerate(bounds):
        part = pl.ds(start, size)
        reads.append(pltpu.make_async_copy(up_hbm.at[part], up_f.at[part], in_sems.at[1 + k]))
    reads.append(pltpu.make_async_copy(prompt_hbm, prompt, in_sems.at[1 + len(bounds)]))
    reads.append(pltpu.make_async_copy(down_hbm, down_f, in_sems.at[2 + len(bounds)]))
    for read in reads[:1 + opening]:
        read.start()

    barrier = pltpu.get_barrier_semaphore()
    for direction in range(4):
        @pl.when(exists[direction])
        def _():
            pl.semaphore_signal(barrier, inc=1, device_id={"fs": me + step[direction]}, device_id_type=MESH)
    for offset in range(1, tp):
        pl.semaphore_signal(barrier, inc=1, device_id={"tp": lax.rem(t + offset, tp)}, device_id_type=MESH)

    def rows_copy(phase, start, size, direction, landing):
        ref = buffers[phase].at[pl.ds(pl.multiple_of(start, size), size)]
        return pltpu.make_async_remote_copy(
            src_ref=ref, dst_ref=ref,
            send_sem=w_send.at[direction, phase], recv_sem=landing,
            device_id={"fs": me + step[direction]}, device_id_type=MESH)

    def weights(phase, block, c, direction):
        slot = (phase * fs + block) * PIECES + c
        return rows_copy(phase, block * rows + c * piece, piece, direction, w_recv.at[slot])

    def send_late(condition, block, direction, kind):
        @pl.when(jnp.logical_and(condition, exists[direction]))
        def _():
            for k in range(CUTS):
                start = block * rows + half * piece + k * cut
                rows_copy(1, start, cut, direction, w_late.at[kind, k]).start()

    def send(condition, phase, block, c, direction):
        @pl.when(jnp.logical_and(condition, exists[direction]))
        def _():
            weights(phase, block, c, direction).start()

    def arrive(condition, phase, block, c):
        @pl.when(condition)
        def _():
            weights(phase, block, c, 0).wait_recv()

    reads[0].wait()
    gain[...] = jnp.transpose(jnp.broadcast_to(gain_row[...], (LANES, rows)))
    always = z >= 0
    for k, (start, size) in enumerate(bounds):
        reads[1 + k].wait()
        if k == opening - 1:
            for read in reads[1 + opening:]:
                read.start()
        where = pl.ds(pl.multiple_of(me * rows + start, size), size)
        for n in range(0, width, LANES):
            up_all[where, n:n + LANES] = (
                gain[start:start + size, :] * up_f[start:start + size, n:n + LANES]).astype(jnp.bfloat16)
        if k == 0:
            pl.semaphore_wait(barrier, sum(e.astype(jnp.int32) for e in exists) + tp - 1)
        for direction in range(4):
            @pl.when(exists[direction])
            def _():
                rows_copy(0, me * rows + start, size, direction, w_recv.at[me * PIECES + start // piece]).start()

    reads[1 + len(bounds)].wait()
    values = prompt[...].astype(jnp.float32)
    scale = lax.rsqrt(jnp.mean(values * values, axis=-1, keepdims=True) + 1e-06)
    mine = pl.ds(pl.multiple_of(t * tokens, tokens), tokens)
    norm_all[mine, :] = (values * scale).astype(jnp.bfloat16)
    reads[2 + len(bounds)].wait()
    for c in range(PIECES):
        where = pl.ds(pl.multiple_of(me * rows + c * piece, piece), piece)
        part = slice(c * piece, (c + 1) * piece)
        down_all[where, :] = down_f[part, :].astype(jnp.bfloat16)

    def token_copy(offset):
        return pltpu.make_async_remote_copy(
            src_ref=norm_all.at[mine], dst_ref=norm_all.at[mine],
            send_sem=n_send.at[offset], recv_sem=n_recv.at[t],
            device_id={"tp": lax.rem(t + offset, tp)}, device_id_type=MESH)

    def token_arrival(offset):
        source = lax.rem(t + offset, tp)
        ref = norm_all.at[pl.ds(pl.multiple_of(source * tokens, tokens), tokens)]
        return pltpu.make_async_remote_copy(
            src_ref=ref, dst_ref=ref, send_sem=n_send.at[offset], recv_sem=n_recv.at[source],
            device_id={"tp": source}, device_id_type=MESH)

    for offset in range(1, tp):
        token_copy(offset).start()
    for c in range(half):
        for direction in (2, 3):
            send(always, 1, me, c, direction)

    def own_down(d):
        for c in range(PIECES):
            if trick and c >= half and d == nz - 2:
                continue
            send(z == d, 1, me, c, 0)
            send(z == nz - 1 - d, 1, me, c, 1)

    def own_late():
        if trick:
            for c in range(half, PIECES):
                send(z == nz - 2, 1, me, c, 0)
                send(z == 1, 1, me, c, 1)

    def own_aside():
        for c in range(half, PIECES):
            for direction in (2, 3):
                send(always, 1, me, c, direction)

    def column(phase, d):
        for c in range(PIECES):
            near = trick and c >= half and d == 1
            for s in (1, -1):
                zb = z + s * d
                there = jnp.logical_and(zb >= 0, zb < nz)
                if near and phase == 1:
                    there = jnp.logical_and(there, exists[1 if s > 0 else 0])
                block = zb * ny + y
                arrive(there, phase, block, c)
                send(there, phase, block, c, 1 if s > 0 else 0)
                if trick and phase == 1 and d == nz - 1 and c >= half:
                    send_late(there, block, 2, 0)
                    send_late(there, block, 3, 0)
                elif not near:
                    send(there, phase, block, c, 2)
                    send(there, phase, block, c, 3)

    def landed():
        for c in range(half, PIECES):
            arrive(z == 0, 1, (z + 1) * ny + y, c)
            arrive(z == nz - 1, 1, (z - 1) * ny + y, c)

    def swap(phase):
        if not trick:
            return
        block = z * ny + 1 - y
        for c in range(half, PIECES):
            if phase == 0:
                arrive(always, phase, block, c)
                send(always, phase, block, c, 0)
                send(always, phase, block, c, 1)
            else:
                send_late(always, block, 0, 2)
                send_late(always, block, 1, 1)

    def sideways(phase, d, s, pieces):
        zb = z + s * d
        inside = jnp.logical_and(zb >= 0, zb < nz)
        for e in range(1, ny):
            for u in (1, -1):
                yb = y + u * e
                there = jnp.logical_and(inside, jnp.logical_and(yb >= 0, yb < ny))
                for c in pieces:
                    if trick and c >= half and (d == 1 or (phase == 0 and d == 0)):
                        continue
                    arrive(there, phase, zb * ny + yb, c)
                    if e < ny - 1:
                        send(there, phase, zb * ny + yb, c, 3 if u > 0 else 2)

    def swapped(phase):
        if trick:
            for c in range(half, PIECES):
                for s in (1, -1):
                    zb = z + s
                    arrive(jnp.logical_and(zb >= 0, zb < nz), phase, zb * ny + 1 - y, c)

    def partial_copy(unit, count, offset):
        peer = lax.rem(t + offset, tp)
        return pltpu.make_async_remote_copy(
            src_ref=part_send.at[pl.ds(unit, count), pl.ds(pl.multiple_of(peer * tokens, tokens), tokens)],
            dst_ref=part_recv.at[t, pl.ds(unit, count)],
            send_sem=p_send.at[offset], recv_sem=p_recv.at[t, 0],
            device_id={"tp": peer}, device_id_type=MESH)

    def arrivals(count):
        for offset in range(1, tp):
            source = lax.rem(t + offset, tp)
            ref = part_recv.at[source, pl.ds(0, count)]
            pltpu.make_async_remote_copy(
                src_ref=ref, dst_ref=ref, send_sem=p_send.at[offset], recv_sem=p_recv.at[source, 0],
                device_id={"tp": source}, device_id_type=MESH).wait_recv()

    def multiply(condition, block, u, count):
        @pl.when(condition)
        def _():
            where = pl.ds(pl.multiple_of(block * rows + u * span, span), count * span)
            unit = block * units + u
            product = lax.dot_general(
                hidden[...], down_all[where, :], (((1,), (1,)), ((), ())),
                preferred_element_type=jnp.float32).astype(jnp.bfloat16)
            for k in range(count):
                part_send[unit + k] = product[:, k * span:(k + 1) * span]
            for offset in range(1, tp):
                partial_copy(unit, count, offset).start()

    def turn(condition, block, u, count):
        if not turned:
            return
        deep = count * span
        wide = TURN // deep if width % (TURN // deep) == 0 else tile

        @pl.when(condition)
        def _():
            where = pl.ds(pl.multiple_of(block * rows + u * span, span), deep)

            @pl.loop(0, width // wide)
            def _(j):
                at = pl.ds(pl.multiple_of(j * wide, wide), wide)
                down_out[at, where] = jnp.transpose(down_all[where, at])

    def consume(condition, block, u, count):
        multiply(condition, block, u, count)
        turn(condition, block, u, count)

    def total_of(unit):
        total = part_send[unit, mine, :].astype(jnp.float32)
        for offset in range(1, tp):
            total += part_recv[lax.rem(t + offset, tp), unit].astype(jnp.float32)
        return total.astype(jnp.bfloat16)

    def add(condition, block, u, count):
        @pl.when(condition)
        def _():
            for k in range(count):
                unit = block * units + u + k
                mixed[:, pl.ds(pl.multiple_of(unit * span, span), span)] = total_of(unit)

    def walk(action, d, aside, first, count):
        across = ny - 1 if aside else 1
        if across * count == 0:
            return

        @pl.loop(0, (1 if d == 0 else 2) * across)
        def _(k):
            zb = z + (1 - 2 * (k // across)) * d
            yb = lax.rem(y + 1 + lax.rem(k, across), ny) if aside else y
            action(jnp.logical_and(zb >= 0, zb < nz), zb * ny + yb, first, count)

    pending = []

    def use(*place):
        walk(consume, *place)
        pending.append(place)

    def finish():
        if span % LANES == 0:
            for place in pending:
                walk(add, *place)
        pending.clear()

    def use_aside(d, first, count):
        for s in signs(d):
            sideways(1, d, s, range(PIECES) if units == 1 else range(first, first + count))
        use(d, True, first, count)

    def signs(d):
        return (1,) if d == 0 else (1, -1)

    def ready(d):
        use(d, False, 0, half if trick and d == 1 else units)
        if d > 0:
            use_aside(d - 1, 0, half if trick and d == 2 else units)

    own_down(0)
    for d in range(1, nz):
        column(0, d)
        if d == 1:
            swap(0)
        own_down(d)
        if d == nz // 2:
            own_aside()
    if nz == 1:
        own_aside()
    else:
        column(1, 1)
    for d in range(nz):
        for s in signs(d):
            sideways(0, d, s, range(PIECES))
    swapped(0)
    for offset in range(1, tp):
        token_arrival(offset).wait_recv()

    @pl.loop(0, width // tile)
    def _(j):
        at = pl.ds(pl.multiple_of(j * tile, tile), tile)
        pre = jnp.dot(norm_all[...], up_all[:, at], preferred_element_type=jnp.float32)
        hidden[:, at] = jnp.square(jnp.maximum(pre, 0.0)).astype(jnp.bfloat16)

    for d in range(min(nz, 2), nz):
        column(1, d)
        if d == nz - 1:
            own_late()
            swap(1)
        if d == 2:
            ready(0)
            ready(1)
        ready(d)
    if nz <= 2:
        for d in range(nz):
            ready(d)
    if trick:
        landed()
        use(1, False, half, units - half)
    if units > 1:
        use_aside(nz - 1, 0, units - 1)
    if trick:
        arrivals(fs * units - 2)
        finish()
        lowest, highest = (z == 0).astype(jnp.int32), (z == nz - 1).astype(jnp.int32)
        inner = 1 - lowest - highest

        def late(slot):
            first = lowest * (nz - 1) + inner * (z - 1)
            block = (first + slot * (z + 1 - 2 * highest - first)) * ny + 1 - y
            return block, 2 * inner + slot * (1 + highest - 2 * inner)

        @pl.loop(0, CUTS)
        def _(k):
            here = pl.ds(pl.multiple_of(k * cut, cut), cut)
            fresh = []
            for slot in range(2):
                block, kind = late(slot)
                start = pl.multiple_of(block * rows + half * piece + k * cut, cut)
                rows_copy(1, start, cut, 0, w_late.at[kind, k]).wait_recv()
                fresh.append(down_all[pl.ds(start, cut), :])
            product = jnp.transpose(lax.dot_general(
                hidden[...], jnp.concatenate(fresh), (((1,), (1,)), ((), ())),
                preferred_element_type=jnp.float32)).astype(jnp.bfloat16)
            for slot in range(2):
                late_send[slot, here, :] = product[slot * cut:(slot + 1) * cut]
            for offset in range(tp - 1, 0, -1):
                peer = lax.rem(t + offset, tp)
                pltpu.make_async_remote_copy(
                    src_ref=late_send.at[:, here, pl.ds(pl.multiple_of(peer * tokens, tokens), tokens)],
                    dst_ref=late_recv.at[t, :, here],
                    send_sem=p_send.at[offset], recv_sem=p_recv.at[t, 1],
                    device_id={"tp": peer}, device_id_type=MESH).start()

        for slot in range(2):
            turn(always, late(slot)[0], half, 1)
        for offset in range(1, tp):
            source = lax.rem(t + offset, tp)
            ref = late_recv.at[source]
            pltpu.make_async_remote_copy(
                src_ref=ref, dst_ref=ref, send_sem=p_send.at[offset], recv_sem=p_recv.at[source, 1],
                device_id={"tp": source}, device_id_type=MESH).wait_recv()
        for slot in range(2):
            total = late_send[slot, :, mine].astype(jnp.float32)
            for offset in range(1, tp):
                total += late_recv[lax.rem(t + offset, tp), slot].astype(jnp.float32)
            column_of = pl.multiple_of(late(slot)[0] * rows + half * piece, piece)
            mixed[:, pl.ds(column_of, piece)] = jnp.transpose(total).astype(jnp.bfloat16)
    else:
        for s in signs(nz - 1):
            sideways(1, nz - 1, s, range(PIECES) if units == 1 else range(units - 1, units))
        use(nz - 1, True, units - 1, 1)
        arrivals(fs * units)
        finish()
    if span % LANES:
        for block in range(fs):
            mixed[:, block * rows:(block + 1) * rows] = total_of(block)

    for offset in range(1, tp):
        token_copy(offset).wait_send()

    for offset in range(1, tp):
        whole = part_recv.at[t]
        pltpu.make_async_remote_copy(
            src_ref=whole, dst_ref=whole, send_sem=p_send.at[offset], recv_sem=p_recv.at[t, 0],
            device_id={"tp": lax.rem(t + offset, tp)}, device_id_type=MESH).wait_send()

    def drain(condition, direction, pieces):
        @pl.when(jnp.logical_and(condition, exists[direction]))
        def _():
            for phase in range(2):
                ref = buffers[phase].at[pl.ds(0, pieces * piece)]
                pltpu.make_async_remote_copy(
                    src_ref=ref, dst_ref=ref, send_sem=w_send.at[direction, phase], recv_sem=w_recv.at[0],
                    device_id={"fs": me + step[direction]}, device_id_type=MESH).wait_send()

    spare = PIECES - half if trick else 0
    for k in range(nz):
        drain(z == k, 0, (k + 1) * PIECES + spare)
        drain(z == k, 1, (nz - k) * PIECES + spare)
        less = spare * ((k > 0) + (k < nz - 1))
        for e in range(ny):
            here = jnp.logical_and(z == k, y == e)
            drain(here, 2, (e + 1) * nz * PIECES - less)
            drain(here, 3, (ny - e) * nz * PIECES - less)


def solution(mesh):
    fs, tp = mesh.shape["fs"], mesh.shape["tp"]
    nz, ny = factor(fs)

    def shards(prompt, norm_gain, up_trained, down_trained):
        rows, width = up_trained.shape
        tokens, depth = prompt.shape
        bf16 = jnp.bfloat16
        turned = turns(rows)
        down_shape = (width, depth) if turned else (depth, width)
        slots = 2 * fs * PIECES
        parts = fs * units_of(rows)
        any_space = pl.BlockSpec(memory_space=pl.ANY)
        vmem = pl.BlockSpec(memory_space=pltpu.VMEM)
        up_whole, down_whole, mixed = pl.pallas_call(
            functools.partial(kernel, nz, ny, tp),
            out_shape=(
                pltpu.VMEM((depth, width), bf16),
                pltpu.VMEM(down_shape, bf16),
                pltpu.VMEM((tokens, depth), bf16),
            ),
            in_specs=[any_space] * 4,
            out_specs=[vmem] * 3,
            scratch_shapes=[
                pltpu.VMEM((tokens, depth), bf16),
                pltpu.VMEM((1, rows), jnp.float32),
                pltpu.VMEM((rows, LANES), jnp.float32),
                pltpu.VMEM((rows, width), jnp.float32),
                pltpu.VMEM((rows, width), jnp.float32),
                pltpu.VMEM((depth, width) if turned else (16, 128), bf16),
                pltpu.VMEM((tp * tokens, depth), bf16),
                pltpu.VMEM((tp * tokens, width), bf16),
                pltpu.VMEM((parts, tp * tokens, depth // parts), bf16),
                pltpu.VMEM((tp, parts, tokens, depth // parts), bf16),
                pltpu.VMEM((2, rows // PIECES, tp * tokens), bf16),
                pltpu.VMEM((tp, 2, rows // PIECES, tokens), bf16),
                pltpu.SemaphoreType.DMA((2 + CUTS + PIECES,)),
                pltpu.SemaphoreType.DMA((4, 2)),
                pltpu.SemaphoreType.DMA((slots,)),
                pltpu.SemaphoreType.DMA((3, CUTS)),
                pltpu.SemaphoreType.DMA((tp,)),
                pltpu.SemaphoreType.DMA((tp,)),
                pltpu.SemaphoreType.DMA((tp,)),
                pltpu.SemaphoreType.DMA((tp, 2)),
            ],
            compiler_params=pltpu.CompilerParams(
                collective_id=0, has_side_effects=True, vmem_limit_bytes=LIMIT * 1024 * 1024
            ),
        )(prompt, norm_gain[None, :], up_trained, down_trained)
        up_whole, down_whole, mixed = pl.pallas_call(
            flush,
            out_shape=(
                jax.ShapeDtypeStruct((depth, width), bf16),
                jax.ShapeDtypeStruct(down_shape, bf16),
                jax.ShapeDtypeStruct((tokens, depth), bf16),
            ),
            in_specs=[vmem] * 3,
            out_specs=[any_space] * 3,
            scratch_shapes=[pltpu.SemaphoreType.DMA((3,))],
            compiler_params=pltpu.CompilerParams(vmem_limit_bytes=2 * 1024 * 1024),
        )(up_whole, down_whole, mixed)
        return up_whole, down_whole if turned else jnp.transpose(down_whole), mixed

    return jax.shard_map(
        shards,
        mesh=mesh,
        in_specs=(P(("fs", "tp"), None), P("fs"), P("fs", "tp"), P("fs", "tp")),
        out_specs=(P(None, "tp"), P("tp", None), P(("fs", "tp"), None)),
        check_vma=False,
    )
```

```python
import functools

import jax
import jax.numpy as jnp
from jax import lax
from jax.experimental import pallas as pl
from jax.experimental.pallas import tpu as pltpu
from jax.sharding import PartitionSpec as P

MESH = pl.DeviceIdType.MESH
PIECES = 2
LIMIT = 40
LANES = 128
CUTS = 8
FLUSHES = 4
TURN = 128 * 1024


def factor(fs):
    ny = 1
    while ny * 2 * ny * 2 <= fs:
        ny *= 2
    return fs // ny, ny


def turns(rows):
    return rows % 128 == 0


def units_of(rows):
    return PIECES if rows // PIECES % LANES == 0 else 1


def flush(up_in, down_in, mixed_in, up_out, down_out, mixed_out, sems):
    copies = []
    for i, (source, target) in enumerate(((up_in, up_out), (down_in, down_out), (mixed_in, mixed_out))):
        deep = source.shape[0] // FLUSHES
        for k in range(FLUSHES):
            part = pl.ds(k * deep, deep)
            copies.append(pltpu.make_async_copy(source.at[part], target.at[part], sems.at[i * FLUSHES + k]))
    for copy in copies:
        copy.start()
    for copy in copies:
        copy.wait()


def kernel(nz, ny, tp, prompt_hbm, gain_hbm, up_hbm, down_hbm, up_all, down_out, mixed,
           prompt, gain_row, gain, up_f, down_f,
           down_scratch, norm_all, hidden, part_send, part_recv, late_send, late_recv,
           in_sems, w_send, w_recv, w_late, joint):
    fs = nz * ny
    rows, width = up_f.shape
    tile = 256
    turned = turns(rows)
    down_all = down_scratch if turned else down_out
    piece = rows // PIECES
    tokens = prompt.shape[0]
    me = lax.axis_index("fs")
    t = lax.axis_index("tp")
    z, y = me // ny, lax.rem(me, ny)
    exists = (z < nz - 1, z > 0, y < ny - 1, y > 0)
    step = (ny, -ny, 1, -1)
    units = units_of(rows)
    span = rows // units
    trick = ny == 2 and nz > 2 and units == PIECES == 2 and tokens % LANES == 0
    cut = piece // CUTS
    opening = CUTS if cut % 16 == 0 else 1
    half = PIECES // 2
    buffers = (up_all, down_all)

    share = piece // opening
    bounds = [(k * share, share) for k in range(opening)]
    bounds += [(c * piece, piece) for c in range(1, PIECES)]
    reads = [pltpu.make_async_copy(gain_hbm, gain_row, in_sems.at[0])]
    for k, (start, size) in enumerate(bounds):
        part = pl.ds(start, size)
        reads.append(pltpu.make_async_copy(up_hbm.at[part], up_f.at[part], in_sems.at[1 + k]))
    reads.append(pltpu.make_async_copy(prompt_hbm, prompt, in_sems.at[1 + len(bounds)]))
    reads.append(pltpu.make_async_copy(down_hbm, down_f, in_sems.at[2 + len(bounds)]))
    for read in reads[:1 + opening]:
        read.start()

    barrier = pltpu.get_barrier_semaphore()
    for direction in range(4):
        @pl.when(exists[direction])
        def _():
            pl.semaphore_signal(barrier, inc=1, device_id={"fs": me + step[direction]}, device_id_type=MESH)
    for offset in range(1, tp):
        pl.semaphore_signal(barrier, inc=1, device_id={"tp": lax.rem(t + offset, tp)}, device_id_type=MESH)

    def rows_copy(phase, start, size, direction, landing):
        ref = buffers[phase].at[pl.ds(pl.multiple_of(start, size), size)]
        return pltpu.make_async_remote_copy(
            src_ref=ref, dst_ref=ref,
            send_sem=w_send.at[direction, phase], recv_sem=landing,
            device_id={"fs": me + step[direction]}, device_id_type=MESH)

    def weights(phase, block, c, direction):
        slot = (phase * fs + block) * PIECES + c
        return rows_copy(phase, block * rows + c * piece, piece, direction, w_recv.at[slot])

    def send_late(condition, block, direction, kind):
        @pl.when(jnp.logical_and(condition, exists[direction]))
        def _():
            for k in range(CUTS):
                start = block * rows + half * piece + k * cut
                rows_copy(1, start, cut, direction, w_late.at[kind, k]).start()

    def send(condition, phase, block, c, direction):
        @pl.when(jnp.logical_and(condition, exists[direction]))
        def _():
            weights(phase, block, c, direction).start()

    def arrive(condition, phase, block, c):
        @pl.when(condition)
        def _():
            weights(phase, block, c, 0).wait_recv()

    reads[0].wait()
    gain[...] = jnp.transpose(jnp.broadcast_to(gain_row[...], (LANES, rows)))
    always = z >= 0
    for k, (start, size) in enumerate(bounds):
        reads[1 + k].wait()
        if k == opening - 1:
            for read in reads[1 + opening:]:
                read.start()
        where = pl.ds(pl.multiple_of(me * rows + start, size), size)
        for n in range(0, width, LANES):
            up_all[where, n:n + LANES] = (
                gain[start:start + size, :] * up_f[start:start + size, n:n + LANES]).astype(jnp.bfloat16)
        if k == 0:
            pl.semaphore_wait(barrier, sum(e.astype(jnp.int32) for e in exists) + tp - 1)
        for direction in range(4):
            @pl.when(exists[direction])
            def _():
                rows_copy(0, me * rows + start, size, direction, w_recv.at[me * PIECES + max(0, k + 1 - opening)]).start()

    reads[1 + len(bounds)].wait()
    values = prompt[...].astype(jnp.float32)
    scale = lax.rsqrt(jnp.mean(values * values, axis=-1, keepdims=True) + 1e-06)
    mine = pl.ds(pl.multiple_of(t * tokens, tokens), tokens)
    norm_all[mine, :] = (values * scale).astype(jnp.bfloat16)
    reads[2 + len(bounds)].wait()
    for c in range(PIECES):
        where = pl.ds(pl.multiple_of(me * rows + c * piece, piece), piece)
        part = slice(c * piece, (c + 1) * piece)
        down_all[where, :] = down_f[part, :].astype(jnp.bfloat16)

    def token_copy(offset):
        return pltpu.make_async_remote_copy(
            src_ref=norm_all.at[mine], dst_ref=norm_all.at[mine],
            send_sem=joint.at[0], recv_sem=joint.at[1],
            device_id={"tp": lax.rem(t + offset, tp)}, device_id_type=MESH)

    def settle(ref, sent, landed_on):
        return pltpu.make_async_remote_copy(
            src_ref=ref, dst_ref=ref, send_sem=joint.at[sent], recv_sem=joint.at[landed_on],
            device_id={"tp": lax.rem(t + 1, tp)}, device_id_type=MESH)

    peers = pl.ds(0, tp - 1)
    tokens_of_peers = norm_all.at[pl.ds(0, (tp - 1) * tokens)]

    for offset in range(1, tp):
        token_copy(offset).start()
    for c in range(half):
        for direction in (2, 3):
            send(always, 1, me, c, direction)

    def own_down(d):
        for c in range(PIECES):
            if trick and c >= half and d == nz - 2:
                continue
            send(z == d, 1, me, c, 0)
            send(z == nz - 1 - d, 1, me, c, 1)

    def own_late():
        if trick:
            for c in range(half, PIECES):
                send(z == nz - 2, 1, me, c, 0)
                send(z == 1, 1, me, c, 1)

    def own_aside():
        for c in range(half, PIECES):
            for direction in (2, 3):
                send(always, 1, me, c, direction)

    def column(phase, d):
        for c in range(PIECES):
            near = trick and c >= half and d == 1
            for s in (1, -1):
                zb = z + s * d
                there = jnp.logical_and(zb >= 0, zb < nz)
                if near and phase == 1:
                    there = jnp.logical_and(there, exists[1 if s > 0 else 0])
                block = zb * ny + y
                arrive(there, phase, block, c)
                send(there, phase, block, c, 1 if s > 0 else 0)
                if trick and phase == 1 and d == nz - 1 and c >= half:
                    send_late(there, block, 2, 0)
                    send_late(there, block, 3, 0)
                elif not near:
                    send(there, phase, block, c, 2)
                    send(there, phase, block, c, 3)

    def landed():
        for c in range(half, PIECES):
            arrive(z == 0, 1, (z + 1) * ny + y, c)
            arrive(z == nz - 1, 1, (z - 1) * ny + y, c)

    def swap(phase):
        if not trick:
            return
        block = z * ny + 1 - y
        for c in range(half, PIECES):
            if phase == 0:
                arrive(always, phase, block, c)
                send(always, phase, block, c, 0)
                send(always, phase, block, c, 1)
            else:
                send_late(always, block, 0, 2)
                send_late(always, block, 1, 1)

    def sideways(phase, d, s, pieces):
        zb = z + s * d
        inside = jnp.logical_and(zb >= 0, zb < nz)
        for e in range(1, ny):
            for u in (1, -1):
                yb = y + u * e
                there = jnp.logical_and(inside, jnp.logical_and(yb >= 0, yb < ny))
                for c in pieces:
                    if trick and c >= half and (d == 1 or (phase == 0 and d == 0)):
                        continue
                    arrive(there, phase, zb * ny + yb, c)
                    if e < ny - 1:
                        send(there, phase, zb * ny + yb, c, 3 if u > 0 else 2)

    def swapped(phase):
        if trick:
            for c in range(half, PIECES):
                for s in (1, -1):
                    zb = z + s
                    arrive(jnp.logical_and(zb >= 0, zb < nz), phase, zb * ny + 1 - y, c)

    def partial_copy(unit, count, offset):
        peer = lax.rem(t + offset, tp)
        return pltpu.make_async_remote_copy(
            src_ref=part_send.at[pl.ds(unit, count), pl.ds(pl.multiple_of(peer * tokens, tokens), tokens)],
            dst_ref=part_recv.at[t, pl.ds(unit, count)],
            send_sem=joint.at[2], recv_sem=joint.at[3],
            device_id={"tp": peer}, device_id_type=MESH)

    def arrivals(count):
        settle(part_recv.at[peers, pl.ds(0, count)], 2, 3).wait_recv()

    def multiply(condition, block, u, count):
        @pl.when(condition)
        def _():
            where = pl.ds(pl.multiple_of(block * rows + u * span, span), count * span)
            unit = block * units + u
            product = lax.dot_general(
                hidden[...], down_all[where, :], (((1,), (1,)), ((), ())),
                preferred_element_type=jnp.float32).astype(jnp.bfloat16)
            for k in range(count):
                part_send[unit + k] = product[:, k * span:(k + 1) * span]
            for offset in range(1, tp):
                partial_copy(unit, count, offset).start()

    def turn(condition, block, u, count):
        if not turned:
            return
        deep = count * span
        wide = TURN // deep if width % (TURN // deep) == 0 else tile

        @pl.when(condition)
        def _():
            where = pl.ds(pl.multiple_of(block * rows + u * span, span), deep)

            @pl.loop(0, width // wide)
            def _(j):
                at = pl.ds(pl.multiple_of(j * wide, wide), wide)
                down_out[at, where] = jnp.transpose(down_all[where, at])

    def consume(condition, block, u, count):
        multiply(condition, block, u, count)
        turn(condition, block, u, count)

    def total_of(unit):
        total = part_send[unit, mine, :].astype(jnp.float32)
        for offset in range(1, tp):
            total += part_recv[lax.rem(t + offset, tp), unit].astype(jnp.float32)
        return total.astype(jnp.bfloat16)

    def add(condition, block, u, count):
        @pl.when(condition)
        def _():
            for k in range(count):
                unit = block * units + u + k
                mixed[:, pl.ds(pl.multiple_of(unit * span, span), span)] = total_of(unit)

    def walk(action, d, aside, first, count):
        across = ny - 1 if aside else 1
        if across * count == 0:
            return

        @pl.loop(0, (1 if d == 0 else 2) * across)
        def _(k):
            zb = z + (1 - 2 * (k // across)) * d
            yb = lax.rem(y + 1 + lax.rem(k, across), ny) if aside else y
            action(jnp.logical_and(zb >= 0, zb < nz), zb * ny + yb, first, count)

    pending = []

    def use(*place):
        walk(consume, *place)
        pending.append(place)

    def finish():
        if span % LANES == 0:
            for place in pending:
                walk(add, *place)
        pending.clear()

    def use_aside(d, first, count):
        for s in signs(d):
            sideways(1, d, s, range(PIECES) if units == 1 else range(first, first + count))
        use(d, True, first, count)

    def signs(d):
        return (1,) if d == 0 else (1, -1)

    def ready(d):
        use(d, False, 0, half if trick and d == 1 else units)
        if d > 0:
            use_aside(d - 1, 0, half if trick and d == 2 else units)

    own_down(0)
    for d in range(1, nz):
        column(0, d)
        if d == 1:
            swap(0)
        own_down(d)
        if d == nz // 2:
            own_aside()
    if nz == 1:
        own_aside()
    else:
        column(1, 1)
    for d in range(nz):
        for s in signs(d):
            sideways(0, d, s, range(PIECES))
    swapped(0)
    settle(tokens_of_peers, 0, 1).wait_recv()

    @pl.loop(0, width // tile)
    def _(j):
        at = pl.ds(pl.multiple_of(j * tile, tile), tile)
        pre = jnp.dot(norm_all[...], up_all[:, at], preferred_element_type=jnp.float32)
        hidden[:, at] = jnp.square(jnp.maximum(pre, 0.0)).astype(jnp.bfloat16)

    for d in range(min(nz, 2), nz):
        column(1, d)
        if d == nz - 1:
            own_late()
            swap(1)
        if d == 2:
            ready(0)
            ready(1)
        ready(d)
    if nz <= 2:
        for d in range(nz):
            ready(d)
    if trick:
        landed()
        use(1, False, half, units - half)
    if units > 1:
        use_aside(nz - 1, 0, units - 1)
    if trick:
        arrivals(fs * units - 2)
        finish()
        lowest, highest = (z == 0).astype(jnp.int32), (z == nz - 1).astype(jnp.int32)
        inner = 1 - lowest - highest

        def late(slot):
            first = lowest * (nz - 1) + inner * (z - 1)
            block = (first + slot * (z + 1 - 2 * highest - first)) * ny + 1 - y
            return block, 2 * inner + slot * (1 + highest - 2 * inner)

        @pl.loop(0, CUTS)
        def _(k):
            here = pl.ds(pl.multiple_of(k * cut, cut), cut)
            fresh = []
            for slot in range(2):
                block, kind = late(slot)
                start = pl.multiple_of(block * rows + half * piece + k * cut, cut)
                rows_copy(1, start, cut, 0, w_late.at[kind, k]).wait_recv()
                fresh.append(down_all[pl.ds(start, cut), :])
            product = jnp.transpose(lax.dot_general(
                hidden[...], jnp.concatenate(fresh), (((1,), (1,)), ((), ())),
                preferred_element_type=jnp.float32)).astype(jnp.bfloat16)
            for slot in range(2):
                late_send[slot, here, :] = product[slot * cut:(slot + 1) * cut]
            for offset in range(tp - 1, 0, -1):
                peer = lax.rem(t + offset, tp)
                pltpu.make_async_remote_copy(
                    src_ref=late_send.at[:, here, pl.ds(pl.multiple_of(peer * tokens, tokens), tokens)],
                    dst_ref=late_recv.at[t, :, here],
                    send_sem=joint.at[2], recv_sem=joint.at[4],
                    device_id={"tp": peer}, device_id_type=MESH).start()

        for slot in range(2):
            turn(always, late(slot)[0], half, 1)
        settle(late_recv.at[peers], 2, 4).wait_recv()
        for slot in range(2):
            total = late_send[slot, :, mine].astype(jnp.float32)
            for offset in range(1, tp):
                total += late_recv[lax.rem(t + offset, tp), slot].astype(jnp.float32)
            column_of = pl.multiple_of(late(slot)[0] * rows + half * piece, piece)
            mixed[:, pl.ds(column_of, piece)] = jnp.transpose(total).astype(jnp.bfloat16)
    else:
        for s in signs(nz - 1):
            sideways(1, nz - 1, s, range(PIECES) if units == 1 else range(units - 1, units))
        use(nz - 1, True, units - 1, 1)
        arrivals(fs * units)
        finish()
    if span % LANES:
        for block in range(fs):
            mixed[:, block * rows:(block + 1) * rows] = total_of(block)

    settle(tokens_of_peers, 0, 1).wait_send()
    settle(part_recv.at[peers], 2, 3).wait_send()

    def drain(condition, direction, blocks, pieces):
        @pl.when(jnp.logical_and(condition, exists[direction]))
        def _():
            for phase in range(2):
                count = blocks * rows + (pieces * piece if trick else 0)
                ref = buffers[phase].at[pl.ds(0, count)]
                pltpu.make_async_remote_copy(
                    src_ref=ref, dst_ref=ref, send_sem=w_send.at[direction, phase], recv_sem=w_recv.at[0],
                    device_id={"fs": me + step[direction]}, device_id_type=MESH).wait_send()

    for k in range(nz):
        drain(z == k, 0, k + 1, 1)
        drain(z == k, 1, nz - k, 1)
        near = (k > 0) + (k < nz - 1)
        for e in range(ny):
            here = jnp.logical_and(z == k, y == e)
            drain(here, 2, (e + 1) * nz, -near)
            drain(here, 3, (ny - e) * nz, -near)


def solution(mesh):
    fs, tp = mesh.shape["fs"], mesh.shape["tp"]
    nz, ny = factor(fs)

    def shards(prompt, norm_gain, up_trained, down_trained):
        rows, width = up_trained.shape
        tokens, depth = prompt.shape
        bf16 = jnp.bfloat16
        turned = turns(rows)
        down_shape = (width, depth) if turned else (depth, width)
        slots = 2 * fs * PIECES
        parts = fs * units_of(rows)
        any_space = pl.BlockSpec(memory_space=pl.ANY)
        vmem = pl.BlockSpec(memory_space=pltpu.VMEM)
        up_whole, down_whole, mixed = pl.pallas_call(
            functools.partial(kernel, nz, ny, tp),
            out_shape=(
                pltpu.VMEM((depth, width), bf16),
                pltpu.VMEM(down_shape, bf16),
                pltpu.VMEM((tokens, depth), bf16),
            ),
            in_specs=[any_space] * 4,
            out_specs=[vmem] * 3,
            scratch_shapes=[
                pltpu.VMEM((tokens, depth), bf16),
                pltpu.VMEM((1, rows), jnp.float32),
                pltpu.VMEM((rows, LANES), jnp.float32),
                pltpu.VMEM((rows, width), jnp.float32),
                pltpu.VMEM((rows, width), jnp.float32),
                pltpu.VMEM((depth, width) if turned else (16, 128), bf16),
                pltpu.VMEM((tp * tokens, depth), bf16),
                pltpu.VMEM((tp * tokens, width), bf16),
                pltpu.VMEM((parts, tp * tokens, depth // parts), bf16),
                pltpu.VMEM((tp, parts, tokens, depth // parts), bf16),
                pltpu.VMEM((2, rows // PIECES, tp * tokens), bf16),
                pltpu.VMEM((tp, 2, rows // PIECES, tokens), bf16),
                pltpu.SemaphoreType.DMA((2 + CUTS + PIECES,)),
                pltpu.SemaphoreType.DMA((4, 2)),
                pltpu.SemaphoreType.DMA((slots,)),
                pltpu.SemaphoreType.DMA((3, CUTS)),
                pltpu.SemaphoreType.DMA((5,)),
            ],
            compiler_params=pltpu.CompilerParams(
                collective_id=0, has_side_effects=True, vmem_limit_bytes=LIMIT * 1024 * 1024
            ),
        )(prompt, norm_gain[None, :], up_trained, down_trained)
        up_whole, down_whole, mixed = pl.pallas_call(
            flush,
            out_shape=(
                jax.ShapeDtypeStruct((depth, width), bf16),
                jax.ShapeDtypeStruct(down_shape, bf16),
                jax.ShapeDtypeStruct((tokens, depth), bf16),
            ),
            in_specs=[vmem] * 3,
            out_specs=[any_space] * 3,
            scratch_shapes=[pltpu.SemaphoreType.DMA((3 * FLUSHES,))],
            compiler_params=pltpu.CompilerParams(vmem_limit_bytes=2 * 1024 * 1024),
        )(up_whole, down_whole, mixed)
        return up_whole, down_whole if turned else jnp.transpose(down_whole), mixed

    return jax.shard_map(
        shards,
        mesh=mesh,
        in_specs=(P(("fs", "tp"), None), P("fs"), P("fs", "tp"), P("fs", "tp")),
        out_specs=(P(None, "tp"), P("tp", None), P(("fs", "tp"), None)),
        check_vma=False,
    )
```

```python
import functools

import jax
import jax.numpy as jnp
from jax import lax
from jax.experimental import pallas as pl
from jax.experimental.pallas import tpu as pltpu
from jax.sharding import PartitionSpec as P

MESH = pl.DeviceIdType.MESH
PIECES = 2
LIMIT = 40
LANES = 128
CUTS = 8
OPENING = 4
FLUSHES = 4
TURN = 128 * 1024


def factor(fs):
    ny = 1
    while ny * 2 * ny * 2 <= fs:
        ny *= 2
    return fs // ny, ny


def turns(rows):
    return rows % 128 == 0


def units_of(rows):
    return PIECES if rows // PIECES % LANES == 0 else 1


def flush(up_in, down_in, mixed_in, up_out, down_out, mixed_out, sems):
    copies = []
    for i, (source, target) in enumerate(((up_in, up_out), (down_in, down_out), (mixed_in, mixed_out))):
        deep = source.shape[0] // FLUSHES
        for k in range(FLUSHES):
            part = pl.ds(k * deep, deep)
            copies.append(pltpu.make_async_copy(source.at[part], target.at[part], sems.at[i * FLUSHES + k]))
    for copy in copies:
        copy.start()
    for copy in copies:
        copy.wait()


def kernel(nz, ny, tp, prompt_hbm, gain_hbm, up_hbm, down_hbm, up_all, down_out, mixed,
           prompt, gain_row, gain, up_f, down_f,
           down_scratch, norm_all, hidden, part_send, part_recv, late_send, late_recv,
           in_sems, w_send, w_recv, w_late, joint):
    fs = nz * ny
    rows, width = up_f.shape
    tile = 256
    turned = turns(rows)
    down_all = down_scratch if turned else down_out
    piece = rows // PIECES
    tokens = prompt.shape[0]
    me = lax.axis_index("fs")
    t = lax.axis_index("tp")
    z, y = me // ny, lax.rem(me, ny)
    exists = (z < nz - 1, z > 0, y < ny - 1, y > 0)
    step = (ny, -ny, 1, -1)
    units = units_of(rows)
    span = rows // units
    trick = ny == 2 and nz > 2 and units == PIECES == 2 and tokens % LANES == 0
    cut = piece // CUTS
    opening = OPENING if piece % (16 * OPENING) == 0 else 1
    half = PIECES // 2
    buffers = (up_all, down_all)

    share = piece // opening
    bounds = [(k * share, share) for k in range(opening)]
    bounds += [(c * piece, piece) for c in range(1, PIECES)]
    reads = [pltpu.make_async_copy(gain_hbm, gain_row, in_sems.at[0])]
    for k, (start, size) in enumerate(bounds):
        part = pl.ds(start, size)
        reads.append(pltpu.make_async_copy(up_hbm.at[part], up_f.at[part], in_sems.at[1 + k]))
    reads.append(pltpu.make_async_copy(prompt_hbm, prompt, in_sems.at[1 + len(bounds)]))
    reads.append(pltpu.make_async_copy(down_hbm, down_f, in_sems.at[2 + len(bounds)]))
    for read in reads[:1 + opening]:
        read.start()

    barrier = pltpu.get_barrier_semaphore()
    for direction in range(4):
        @pl.when(exists[direction])
        def _():
            pl.semaphore_signal(barrier, inc=1, device_id={"fs": me + step[direction]}, device_id_type=MESH)
    for offset in range(1, tp):
        pl.semaphore_signal(barrier, inc=1, device_id={"tp": lax.rem(t + offset, tp)}, device_id_type=MESH)

    def rows_copy(phase, start, size, direction, landing):
        ref = buffers[phase].at[pl.ds(pl.multiple_of(start, size), size)]
        return pltpu.make_async_remote_copy(
            src_ref=ref, dst_ref=ref,
            send_sem=w_send.at[direction, phase], recv_sem=landing,
            device_id={"fs": me + step[direction]}, device_id_type=MESH)

    def weights(phase, block, c, direction):
        slot = (phase * fs + block) * PIECES + c
        return rows_copy(phase, block * rows + c * piece, piece, direction, w_recv.at[slot])

    def send_late(condition, block, direction, kind):
        @pl.when(jnp.logical_and(condition, exists[direction]))
        def _():
            for k in range(CUTS):
                start = block * rows + half * piece + k * cut
                rows_copy(1, start, cut, direction, w_late.at[kind, k]).start()

    def send(condition, phase, block, c, direction):
        @pl.when(jnp.logical_and(condition, exists[direction]))
        def _():
            weights(phase, block, c, direction).start()

    def arrive(condition, phase, block, c):
        @pl.when(condition)
        def _():
            weights(phase, block, c, 0).wait_recv()

    reads[0].wait()
    gain[...] = jnp.transpose(jnp.broadcast_to(gain_row[...], (LANES, rows)))
    always = z >= 0
    for k, (start, size) in enumerate(bounds):
        reads[1 + k].wait()
        if k == opening - 1:
            for read in reads[1 + opening:]:
                read.start()
        where = pl.ds(pl.multiple_of(me * rows + start, size), size)
        for n in range(0, width, LANES):
            up_all[where, n:n + LANES] = (
                gain[start:start + size, :] * up_f[start:start + size, n:n + LANES]).astype(jnp.bfloat16)
        if k == 0:
            pl.semaphore_wait(barrier, sum(e.astype(jnp.int32) for e in exists) + tp - 1)
        for direction in range(4):
            @pl.when(exists[direction])
            def _():
                rows_copy(0, me * rows + start, size, direction, w_recv.at[me * PIECES + max(0, k + 1 - opening)]).start()

    reads[1 + len(bounds)].wait()
    values = prompt[...].astype(jnp.float32)
    scale = lax.rsqrt(jnp.mean(values * values, axis=-1, keepdims=True) + 1e-06)
    mine = pl.ds(pl.multiple_of(t * tokens, tokens), tokens)
    norm_all[mine, :] = (values * scale).astype(jnp.bfloat16)
    reads[2 + len(bounds)].wait()
    for c in range(PIECES):
        where = pl.ds(pl.multiple_of(me * rows + c * piece, piece), piece)
        part = slice(c * piece, (c + 1) * piece)
        down_all[where, :] = down_f[part, :].astype(jnp.bfloat16)

    def token_copy(offset):
        return pltpu.make_async_remote_copy(
            src_ref=norm_all.at[mine], dst_ref=norm_all.at[mine],
            send_sem=joint.at[0], recv_sem=joint.at[1],
            device_id={"tp": lax.rem(t + offset, tp)}, device_id_type=MESH)

    def settle(ref, sent, landed_on):
        return pltpu.make_async_remote_copy(
            src_ref=ref, dst_ref=ref, send_sem=joint.at[sent], recv_sem=joint.at[landed_on],
            device_id={"tp": lax.rem(t + 1, tp)}, device_id_type=MESH)

    peers = pl.ds(0, tp - 1)
    tokens_of_peers = norm_all.at[pl.ds(0, (tp - 1) * tokens)]

    for offset in range(1, tp):
        token_copy(offset).start()
    for c in range(half):
        for direction in (2, 3):
            send(always, 1, me, c, direction)

    def own_down(d):
        for c in range(PIECES):
            if trick and c >= half and d == nz - 2:
                continue
            send(z == d, 1, me, c, 0)
            send(z == nz - 1 - d, 1, me, c, 1)

    def own_late():
        if trick:
            for c in range(half, PIECES):
                send(z == nz - 2, 1, me, c, 0)
                send(z == 1, 1, me, c, 1)

    def own_aside():
        for c in range(half, PIECES):
            for direction in (2, 3):
                send(always, 1, me, c, direction)

    def column(phase, d):
        for c in range(PIECES):
            near = trick and c >= half and d == 1
            for s in (1, -1):
                zb = z + s * d
                there = jnp.logical_and(zb >= 0, zb < nz)
                if near and phase == 1:
                    there = jnp.logical_and(there, exists[1 if s > 0 else 0])
                block = zb * ny + y
                arrive(there, phase, block, c)
                send(there, phase, block, c, 1 if s > 0 else 0)
                if trick and phase == 1 and d == nz - 1 and c >= half:
                    send_late(there, block, 2, 0)
                    send_late(there, block, 3, 0)
                elif not near:
                    send(there, phase, block, c, 2)
                    send(there, phase, block, c, 3)

    def landed():
        for c in range(half, PIECES):
            arrive(z == 0, 1, (z + 1) * ny + y, c)
            arrive(z == nz - 1, 1, (z - 1) * ny + y, c)

    def swap(phase):
        if not trick:
            return
        block = z * ny + 1 - y
        for c in range(half, PIECES):
            if phase == 0:
                arrive(always, phase, block, c)
                send(always, phase, block, c, 0)
                send(always, phase, block, c, 1)
            else:
                send_late(always, block, 0, (z == nz - 2).astype(jnp.int32))
                send_late(always, block, 1, 1)

    def sideways(phase, d, s, pieces):
        zb = z + s * d
        inside = jnp.logical_and(zb >= 0, zb < nz)
        for e in range(1, ny):
            for u in (1, -1):
                yb = y + u * e
                there = jnp.logical_and(inside, jnp.logical_and(yb >= 0, yb < ny))
                for c in pieces:
                    if trick and c >= half and (d == 1 or (phase == 0 and d == 0)):
                        continue
                    arrive(there, phase, zb * ny + yb, c)
                    if e < ny - 1:
                        send(there, phase, zb * ny + yb, c, 3 if u > 0 else 2)

    def swapped(phase):
        if trick:
            for c in range(half, PIECES):
                for s in (1, -1):
                    zb = z + s
                    arrive(jnp.logical_and(zb >= 0, zb < nz), phase, zb * ny + 1 - y, c)

    def partial_copy(unit, count, offset):
        peer = lax.rem(t + offset, tp)
        return pltpu.make_async_remote_copy(
            src_ref=part_send.at[pl.ds(unit, count), pl.ds(pl.multiple_of(peer * tokens, tokens), tokens)],
            dst_ref=part_recv.at[t, pl.ds(unit, count)],
            send_sem=joint.at[2], recv_sem=joint.at[3],
            device_id={"tp": peer}, device_id_type=MESH)

    def arrivals(count):
        settle(part_recv.at[peers, pl.ds(0, count)], 2, 3).wait_recv()

    def multiply(condition, block, u, count):
        @pl.when(condition)
        def _():
            where = pl.ds(pl.multiple_of(block * rows + u * span, span), count * span)
            unit = block * units + u
            product = lax.dot_general(
                hidden[...], down_all[where, :], (((1,), (1,)), ((), ())),
                preferred_element_type=jnp.float32).astype(jnp.bfloat16)
            for k in range(count):
                part_send[unit + k] = product[:, k * span:(k + 1) * span]
            for offset in range(1, tp):
                partial_copy(unit, count, offset).start()

    def turn(condition, block, u, count):
        if not turned:
            return
        deep = count * span
        wide = TURN // deep if width % (TURN // deep) == 0 else tile

        @pl.when(condition)
        def _():
            where = pl.ds(pl.multiple_of(block * rows + u * span, span), deep)

            @pl.loop(0, width // wide)
            def _(j):
                at = pl.ds(pl.multiple_of(j * wide, wide), wide)
                down_out[at, where] = jnp.transpose(down_all[where, at])

    def consume(condition, block, u, count):
        multiply(condition, block, u, count)
        turn(condition, block, u, count)

    def total_of(unit):
        total = part_send[unit, mine, :].astype(jnp.float32)
        for offset in range(1, tp):
            total += part_recv[lax.rem(t + offset, tp), unit].astype(jnp.float32)
        return total.astype(jnp.bfloat16)

    def add(condition, block, u, count):
        @pl.when(condition)
        def _():
            for k in range(count):
                unit = block * units + u + k
                mixed[:, pl.ds(pl.multiple_of(unit * span, span), span)] = total_of(unit)

    def walk(action, d, aside, first, count):
        across = ny - 1 if aside else 1
        if across * count == 0:
            return

        @pl.loop(0, (1 if d == 0 else 2) * across)
        def _(k):
            zb = z + (1 - 2 * (k // across)) * d
            yb = lax.rem(y + 1 + lax.rem(k, across), ny) if aside else y
            action(jnp.logical_and(zb >= 0, zb < nz), zb * ny + yb, first, count)

    pending = []

    def use(*place):
        walk(consume, *place)
        pending.append(place)

    def finish():
        if span % LANES == 0:
            for place in pending:
                walk(add, *place)
        pending.clear()

    def use_aside(d, first, count):
        for s in signs(d):
            sideways(1, d, s, range(PIECES) if units == 1 else range(first, first + count))
        use(d, True, first, count)

    def signs(d):
        return (1,) if d == 0 else (1, -1)

    def ready(d):
        use(d, False, 0, half if trick and d == 1 else units)
        if d > 0:
            use_aside(d - 1, 0, half if trick and d == 2 else units)

    own_down(0)
    for d in range(1, nz):
        column(0, d)
        if d == 1:
            swap(0)
        own_down(d)
        if d == nz // 2:
            own_aside()
    if nz == 1:
        own_aside()
    else:
        column(1, 1)
    for d in range(nz):
        for s in signs(d):
            sideways(0, d, s, range(PIECES))
    swapped(0)
    settle(tokens_of_peers, 0, 1).wait_recv()

    @pl.loop(0, width // tile)
    def _(j):
        at = pl.ds(pl.multiple_of(j * tile, tile), tile)
        pre = jnp.dot(norm_all[...], up_all[:, at], preferred_element_type=jnp.float32)
        hidden[:, at] = jnp.square(jnp.maximum(pre, 0.0)).astype(jnp.bfloat16)

    for d in range(min(nz, 2), nz):
        column(1, d)
        if d == nz - 1:
            own_late()
            swap(1)
        if d == 2:
            ready(0)
            ready(1)
        ready(d)
    if nz <= 2:
        for d in range(nz):
            ready(d)
    if trick:
        landed()
        use(1, False, half, units - half)
    if units > 1:
        use_aside(nz - 1, 0, units - 1)
    if trick:
        arrivals(fs * units - 2)
        finish()
        lowest, highest = (z == 0).astype(jnp.int32), (z == nz - 1).astype(jnp.int32)
        inner = 1 - lowest - highest

        def late(slot):
            first = lowest * (nz - 1) + inner * (z - 1)
            block = (first + slot * (z + 1 - 2 * highest - first)) * ny + 1 - y
            return block

        @pl.loop(0, CUTS)
        def _(k):
            here = pl.ds(pl.multiple_of(k * cut, cut), cut)
            fresh = []
            for slot in range(2):
                block = late(slot)
                start = pl.multiple_of(block * rows + half * piece + k * cut, cut)
                rows_copy(1, start, cut, 0, w_late.at[slot, k]).wait_recv()
                fresh.append(down_all[pl.ds(start, cut), :])
            product = jnp.transpose(lax.dot_general(
                hidden[...], jnp.concatenate(fresh), (((1,), (1,)), ((), ())),
                preferred_element_type=jnp.float32)).astype(jnp.bfloat16)
            for slot in range(2):
                late_send[slot, here, :] = product[slot * cut:(slot + 1) * cut]
            for offset in range(tp - 1, 0, -1):
                peer = lax.rem(t + offset, tp)
                pltpu.make_async_remote_copy(
                    src_ref=late_send.at[:, here, pl.ds(pl.multiple_of(peer * tokens, tokens), tokens)],
                    dst_ref=late_recv.at[t, :, here],
                    send_sem=joint.at[2], recv_sem=joint.at[4],
                    device_id={"tp": peer}, device_id_type=MESH).start()

        for slot in range(2):
            turn(always, late(slot), half, 1)
        settle(late_recv.at[peers], 2, 4).wait_recv()
        for slot in range(2):
            total = late_send[slot, :, mine].astype(jnp.float32)
            for offset in range(1, tp):
                total += late_recv[lax.rem(t + offset, tp), slot].astype(jnp.float32)
            column_of = pl.multiple_of(late(slot) * rows + half * piece, piece)
            mixed[:, pl.ds(column_of, piece)] = jnp.transpose(total).astype(jnp.bfloat16)
    else:
        for s in signs(nz - 1):
            sideways(1, nz - 1, s, range(PIECES) if units == 1 else range(units - 1, units))
        use(nz - 1, True, units - 1, 1)
        arrivals(fs * units)
        finish()
    if span % LANES:
        for block in range(fs):
            mixed[:, block * rows:(block + 1) * rows] = total_of(block)

    settle(tokens_of_peers, 0, 1).wait_send()
    settle(part_recv.at[peers], 2, 3).wait_send()

    def drain(condition, direction, blocks, pieces):
        @pl.when(jnp.logical_and(condition, exists[direction]))
        def _():
            for phase in range(2):
                count = blocks * rows + (pieces * piece if trick else 0)
                ref = buffers[phase].at[pl.ds(0, count)]
                pltpu.make_async_remote_copy(
                    src_ref=ref, dst_ref=ref, send_sem=w_send.at[direction, phase], recv_sem=w_recv.at[0],
                    device_id={"fs": me + step[direction]}, device_id_type=MESH).wait_send()

    for k in range(nz):
        drain(z == k, 0, k + 1, 1)
        drain(z == k, 1, nz - k, 1)
        near = (k > 0) + (k < nz - 1)
        for e in range(ny):
            here = jnp.logical_and(z == k, y == e)
            drain(here, 2, (e + 1) * nz, -near)
            drain(here, 3, (ny - e) * nz, -near)


def solution(mesh):
    fs, tp = mesh.shape["fs"], mesh.shape["tp"]
    nz, ny = factor(fs)

    def shards(prompt, norm_gain, up_trained, down_trained):
        rows, width = up_trained.shape
        tokens, depth = prompt.shape
        bf16 = jnp.bfloat16
        turned = turns(rows)
        down_shape = (width, depth) if turned else (depth, width)
        slots = 2 * fs * PIECES
        parts = fs * units_of(rows)
        any_space = pl.BlockSpec(memory_space=pl.ANY)
        vmem = pl.BlockSpec(memory_space=pltpu.VMEM)
        up_whole, down_whole, mixed = pl.pallas_call(
            functools.partial(kernel, nz, ny, tp),
            out_shape=(
                pltpu.VMEM((depth, width), bf16),
                pltpu.VMEM(down_shape, bf16),
                pltpu.VMEM((tokens, depth), bf16),
            ),
            in_specs=[any_space] * 4,
            out_specs=[vmem] * 3,
            scratch_shapes=[
                pltpu.VMEM((tokens, depth), bf16),
                pltpu.VMEM((1, rows), jnp.float32),
                pltpu.VMEM((rows, LANES), jnp.float32),
                pltpu.VMEM((rows, width), jnp.float32),
                pltpu.VMEM((rows, width), jnp.float32),
                pltpu.VMEM((depth, width) if turned else (16, 128), bf16),
                pltpu.VMEM((tp * tokens, depth), bf16),
                pltpu.VMEM((tp * tokens, width), bf16),
                pltpu.VMEM((parts, tp * tokens, depth // parts), bf16),
                pltpu.VMEM((tp, parts, tokens, depth // parts), bf16),
                pltpu.VMEM((2, rows // PIECES, tp * tokens), bf16),
                pltpu.VMEM((tp, 2, rows // PIECES, tokens), bf16),
                pltpu.SemaphoreType.DMA((2 + OPENING + PIECES,)),
                pltpu.SemaphoreType.DMA((4, 2)),
                pltpu.SemaphoreType.DMA((slots,)),
                pltpu.SemaphoreType.DMA((2, CUTS)),
                pltpu.SemaphoreType.DMA((5,)),
            ],
            compiler_params=pltpu.CompilerParams(
                collective_id=0, has_side_effects=True, vmem_limit_bytes=LIMIT * 1024 * 1024
            ),
        )(prompt, norm_gain[None, :], up_trained, down_trained)
        up_whole, down_whole, mixed = pl.pallas_call(
            flush,
            out_shape=(
                jax.ShapeDtypeStruct((depth, width), bf16),
                jax.ShapeDtypeStruct(down_shape, bf16),
                jax.ShapeDtypeStruct((tokens, depth), bf16),
            ),
            in_specs=[vmem] * 3,
            out_specs=[any_space] * 3,
            scratch_shapes=[pltpu.SemaphoreType.DMA((3 * FLUSHES,))],
            compiler_params=pltpu.CompilerParams(vmem_limit_bytes=2 * 1024 * 1024),
        )(up_whole, down_whole, mixed)
        return up_whole, down_whole if turned else jnp.transpose(down_whole), mixed

    return jax.shard_map(
        shards,
        mesh=mesh,
        in_specs=(P(("fs", "tp"), None), P("fs"), P("fs", "tp"), P("fs", "tp")),
        out_specs=(P(None, "tp"), P("tp", None), P(("fs", "tp"), None)),
        check_vma=False,
    )
```
